32 devices in a mesh: sp: 8 (over z, x), tp: 4 (over y, core).
Axes of the slice: x: 2, y: 2, z: 4, core: 2. Of those that a mesh axis runs over, the one named last changes fastest.
Arguments:
- stream: bfloat16 [1024, 2048], P('sp', 'tp'), may hold values from -6 to 6
- norm_gain: float32 [2048], replicated, may hold values from 0.1 to 1.9
- w_query: bfloat16 [2048, 1024], P('sp', 'tp'), may hold values from -0.75 to 0.75
- w_key: bfloat16 [2048, 256], P('sp', 'tp'), may hold values from -0.125 to 0.125
- w_value: bfloat16 [2048, 256], P('sp', 'tp'), may hold values from -0.125 to 0.125
- w_conv_in: bfloat16 [2048, 1024], P('sp', 'tp'), may hold values from -0.125 to 0.125
- w_conv_gate: bfloat16 [2048, 1024], P('sp', 'tp'), may hold values from -0.125 to 0.125
- conv_taps: float32 [3, 1024], P(None, 'tp'), may hold values from -3.5 to 3.5
- sb_bias: float32 [16], P('tp'), may hold values from -28 to -13
- w_out_attn: bfloat16 [1024, 2048], P('tp', 'sp'), may hold values from -0.5 to 0.5
- w_out_conv: bfloat16 [1024, 2048], P('tp', 'sp'), may hold values from -0.125 to 0.125
Outputs:
- mixed: bfloat16 [1024, 2048], P('sp', 'tp')
- log_weight_sum: float32 [16, 1024], P('tp', 'sp')
The draws below stay inside these ranges and needn't reach their ends.
All inputs are finite; a program needn't handle non-finite values.
Results may differ from the reference program's by a relative error of at most 0.013.
The reference program's roundings to bfloat16 on the way count: a program that leaves them out, or rounds other values in their place, can miss the bound.
Values may be sent and summed in bfloat16 or wider, within the bound.
A program may use at most 64 MiB of HBM per device.

```python
import math
import jax
import jax.numpy as jnp
from jax import lax

D = 2048
HEADS = 16
HEAD = 64
KV_HEADS = 4
CONV = 1024
CONV_K = 3
SEQ = 1024
N_TP = 4


def draw_sb_bias(key, part):
    pick_key, slow_key, fast_key = jax.random.split(jax.random.fold_in(key, 11), 3)
    reach = math.sqrt(2.0 * math.log(SEQ)) - 0.4
    share = 0.5
    quick = jax.random.uniform(pick_key, (HEADS,), jnp.float32) < share
    slow = -6.0 * reach + jax.random.uniform(slow_key, (HEADS,), jnp.float32, -1.0, 1.0)
    fast = -14.0 + jax.random.uniform(fast_key, (HEADS,), jnp.float32, -1.0, 1.0)
    return jnp.where(quick, fast, slow).astype(jnp.float32)


def steps_of(own_key, shape, pieces, low, high):
    factor_of, own = 1.0, jax.random.fold_in(own_key, 6)
    for dim, shards_of in pieces:
        steps = jnp.exp(jax.random.uniform(jax.random.fold_in(own, dim), (shards_of,), jnp.float32, low / len(pieces), high / len(pieces)))
        factor_of = factor_of * jnp.repeat(steps, shape[dim] // shards_of).reshape([-1 if axis == dim else 1 for axis in range(len(shape))])
    return factor_of


def scatter_about(rng, dims, width, most, cuts=(), kind=jnp.bfloat16):
    array = width * jax.random.normal(rng, dims, jnp.float32)
    if cuts:
        array = array * steps_of(rng, dims, cuts, -0.22, 0.18)
    return jnp.clip(array, -most, most).astype(kind)


def setup_inputs(seed: int = 0) -> dict:
    streams_of = jax.random.split(jax.random.key(seed), 12)
    return {
        "stream": scatter_about(streams_of[0], (SEQ, D), 1.0, 6.0, ((0, 8), (1, 4))),
        "norm_gain": jnp.clip(1.0 + 0.18 * jax.random.normal(streams_of[1], (D,), jnp.float32), 0.1, 1.9),
        "w_query": scatter_about(streams_of[2], (D, HEADS * HEAD), (D // 36) ** -0.5, 0.75, ((0, 8), (1, 4))),
        "w_key": scatter_about(streams_of[3], (D, KV_HEADS * HEAD), D ** -0.5, 0.125, ((0, 8), (1, 4))),
        "w_value": scatter_about(streams_of[4], (D, KV_HEADS * HEAD), D ** -0.5, 0.125, ((0, 8), (1, 4))),
        "w_conv_in": scatter_about(streams_of[5], (D, CONV), D ** -0.5, 0.125, ((0, 8), (1, 4))),
        "w_conv_gate": scatter_about(streams_of[6], (D, CONV), D ** -0.5, 0.125, ((0, 8), (1, 4))),
        "conv_taps": scatter_about(streams_of[7], (CONV_K, CONV), CONV_K ** -0.5, 3.5, ((1, 4),), jnp.float32),
        "sb_bias": draw_sb_bias(jax.random.fold_in(streams_of[11], 71), 0),
        "w_out_attn": scatter_about(streams_of[9], (HEADS * HEAD, D), (HEADS * HEAD // 8) ** -0.5, 0.5, ((0, 4), (1, 8))),
        "w_out_conv": scatter_about(streams_of[10], (CONV, D), (2 * CONV) ** -0.5, 0.125, ((0, 4), (1, 8))),
    }


EPS = 1e-06
FLOOR = 0.02

def project(scaled, weight, row_scale):
    return (jnp.dot(scaled, weight, preferred_element_type=jnp.float32) * row_scale).astype(jnp.bfloat16)

def reference(stream, norm_gain, w_query, w_key, w_value, w_conv_in, w_conv_gate, conv_taps, sb_bias, w_out_attn, w_out_conv):
    stream_f = stream.astype(jnp.float32)
    row_scale = lax.rsqrt(lax.optimization_barrier(jnp.mean(stream_f * stream_f, axis=1, keepdims=True)) + EPS)
    scaled = (stream_f * norm_gain[None, :]).astype(jnp.bfloat16)
    query = project(scaled, w_query, row_scale)
    key = project(scaled, w_key, row_scale)
    value = project(scaled, w_value, row_scale)
    conv_in = project(scaled, w_conv_in, row_scale)
    conv_gate = project(scaled, w_conv_gate, row_scale)
    group = HEADS // KV_HEADS
    queries = query.reshape(SEQ, HEADS, HEAD).transpose(1, 0, 2).astype(jnp.float32)
    keys = jnp.repeat(key.reshape(SEQ, KV_HEADS, HEAD).transpose(1, 0, 2), group, axis=0).astype(jnp.float32)
    values = jnp.repeat(value.reshape(SEQ, KV_HEADS, HEAD).transpose(1, 0, 2), group, axis=0).astype(jnp.float32)
    block = min(512, SEQ)
    blocks = SEQ // block
    score_scale = HEAD ** (-0.5)

    def query_block(block_index):
        begin = (block_index * block).astype(jnp.int32)
        query_rows = lax.dynamic_slice_in_dim(queries, begin, block, 1)
        query_pos = begin + jnp.arange(block, dtype=jnp.int32)

        def turn(step, carry):
            totals, survival = carry
            start = ((block_index - step) * block).astype(jnp.int32)
            key_rows = lax.dynamic_slice_in_dim(keys, start, block, 1)
            value_rows = lax.dynamic_slice_in_dim(values, start, block, 1)
            key_pos = start + jnp.arange(block, dtype=jnp.int32)
            causal = (key_pos[None, :] < query_pos[:, None])[None]
            scores = jnp.einsum('hqd,hkd->hqk', query_rows, key_rows) * score_scale + sb_bias[:, None, None]
            fails = jnp.where(causal, jax.nn.log_sigmoid(-scores), 0.0)
            later = lax.cumsum(fails, axis=2, reverse=True) - fails + survival[:, :, None]
            stick = jnp.where(causal, jnp.exp(jax.nn.log_sigmoid(scores) + later), 0.0)
            stick = lax.optimization_barrier(stick.astype(jnp.bfloat16)).astype(jnp.float32)
            totals = totals + jnp.einsum('hqk,hkd->hqd', stick, value_rows)
            return (totals, survival + lax.optimization_barrier(jnp.sum(fails, axis=2)))
        start_state = (jnp.zeros((HEADS, block, HEAD), jnp.float32), jnp.zeros((HEADS, block), jnp.float32))
        return lax.fori_loop(0, block_index + 1, turn, start_state)
    totals, survival = lax.map(query_block, jnp.arange(blocks, dtype=jnp.int32))
    attended = totals.transpose(1, 0, 2, 3).reshape(HEADS, SEQ, HEAD).astype(jnp.bfloat16)
    survival = survival.transpose(1, 0, 2).reshape(HEADS, SEQ)
    log_weight_sum = jnp.log(jnp.maximum(-jnp.expm1(survival), FLOOR))
    padded = jnp.pad(conv_in.astype(jnp.float32), ((CONV_K - 1, 0), (0, 0)))
    conv_mixed = jnp.zeros((SEQ, CONV), jnp.float32)
    for tap in range(CONV_K):
        conv_mixed = conv_mixed + conv_taps[tap][None, :] * padded[tap:tap + SEQ]
    conv_out = (conv_gate.astype(jnp.float32) * conv_mixed).astype(jnp.bfloat16)
    attended_rows = attended.transpose(1, 0, 2).reshape(SEQ, HEADS * HEAD)
    attn_width = HEADS * HEAD // N_TP
    conv_width = CONV // N_TP
    summed = jnp.zeros((SEQ, D), jnp.float32)
    for group_index in range(N_TP):
        lower = group_index * attn_width
        conv_lower = group_index * conv_width
        partial_value = jnp.dot(attended_rows[:, lower:lower + attn_width], w_out_attn[lower:lower + attn_width], preferred_element_type=jnp.float32)
        partial_value = partial_value + jnp.dot(conv_out[:, conv_lower:conv_lower + conv_width], w_out_conv[conv_lower:conv_lower + conv_width], preferred_element_type=jnp.float32)
        summed = summed + lax.optimization_barrier(partial_value.astype(jnp.bfloat16)).astype(jnp.float32)
    return (summed.astype(jnp.bfloat16), log_weight_sum)
```

```python
import functools

import jax
import jax.numpy as jnp
from jax import lax
from jax.experimental import pallas as pl
from jax.experimental.pallas import tpu as pltpu
from jax.sharding import PartitionSpec as P

HEAD = 64
CONV_K = 3
EPS = 1e-06
FLOOR = 0.02
MESH = pl.DeviceIdType.MESH
F32 = jnp.float32
BF16 = jnp.bfloat16


def kernel(n, groups, inner, heads,
           bias_ref, stream_ref, gain_ref, taps_ref, wq_ref, wci_ref, wcg_ref, wkv_ref, woa_ref, woc_ref,
           out_ref, lws_ref,
           xbuf, scaled, wbuf, wobuf, kvbuf, qbuf, gate, cin, halo, mix, carry, acc, pbuf, rbuf,
           lsem, xsend, xrecv, wup, wdn, wx, wrecv, oup, odn, ox, orecv, ksend, krecv, hsem, psend, precv):
    me, tp = lax.axis_index("sp"), lax.axis_index("tp")
    outer = n // inner
    o, i = me // inner, lax.rem(me, inner)
    rows, tokens = wq_ref.shape[0], stream_ref.shape[0]
    features = stream_ref.shape[1]
    width = wq_ref.shape[1]
    conv = wci_ref.shape[1]
    arows = woa_ref.shape[0]
    per = n // groups

    def wrows(block):
        return pl.ds(pl.multiple_of(block * rows, rows), rows)

    own = wbuf.at[wrows(me)]
    local = [
        (wq_ref, own.at[:, 0:width]),
        (wci_ref, own.at[:, width:width + conv]),
        (wcg_ref, own.at[:, width + conv:width + 2 * conv]),
        (wkv_ref, own.at[:, width + 2 * conv:width + 2 * conv + 2 * HEAD]),
        (stream_ref, xbuf.at[tp]),
        (woa_ref, wobuf.at[me, 0:arows]),
        (woc_ref, wobuf.at[me, arows:2 * arows]),
    ]
    local = [pltpu.make_async_copy(src, dst, lsem.at[j]) for j, (src, dst) in enumerate(local)]
    for copy in local:
        copy.start()

    barrier = pltpu.get_barrier_semaphore()

    def greet(d, _):
        pl.semaphore_signal(barrier, inc=1, device_id={"sp": lax.rem(me + d, n)}, device_id_type=MESH)
        return 0

    lax.fori_loop(1, n, greet, 0)
    for d in range(1, groups):
        pl.semaphore_signal(barrier, inc=1, device_id={"tp": lax.rem(tp + d, groups)}, device_id_type=MESH)
    pl.semaphore_wait(barrier, n - 1 + groups - 1)

    def relay_set(view, up, dn, xs, recv):
        def to(block, sem, oo, ii):
            return pltpu.make_async_remote_copy(
                src_ref=view(block), dst_ref=view(block), send_sem=sem.at[block], recv_sem=recv.at[block],
                device_id={"sp": oo * inner + ii}, device_id_type=MESH)

        def at(oo):
            return oo * inner + i

        def x_each(f):
            for d in range(1, inner):
                f(d)

        def start_up(block):
            @pl.when(o < outer - 1)
            def _():
                to(block, up, o + 1, i).start()

        def start_dn(block):
            @pl.when(o > 0)
            def _():
                to(block, dn, o - 1, i).start()

        def start_x(block):
            x_each(lambda d: to(block, xs.at[d - 1], o, lax.rem(i + d, inner)).start())

        def begin():
            start_up(me)
            start_dn(me)
            start_x(me)

        def step(k):
            @pl.when(o - k >= 0)
            def _():
                block = at(o - k)
                to(block, up, o, i).wait_recv()
                start_up(block)
                start_x(block)

            @pl.when(o + k < outer)
            def _():
                block = at(o + k)
                to(block, dn, o, i).wait_recv()
                start_dn(block)
                start_x(block)

        def finish():
            def each(oo, _):
                block = at(oo)
                x_each(lambda d: to(block, xs.at[d - 1], o, i).wait_send())
                x_each(lambda d: to(oo * inner + lax.rem(i + d, inner), up, o, i).wait_recv())

                @pl.when(jnp.logical_and(oo <= o, o < outer - 1))
                def _():
                    to(block, up, o, i).wait_send()

                @pl.when(jnp.logical_and(oo >= o, o > 0))
                def _():
                    to(block, dn, o, i).wait_send()
                return 0

            lax.fori_loop(0, outer, each, 0)

        return begin, step, finish

    w_begin, w_step, w_finish = relay_set(lambda b: wbuf.at[wrows(b)], wup, wdn, wx, wrecv)
    o_begin, o_step, o_finish = relay_set(lambda b: wobuf.at[b], oup, odn, ox, orecv)

    def steps(step, first, last):
        lax.fori_loop(first, last, lambda k, c: (step(k), c)[1], 0)

    for copy in local:
        copy.wait()
    w_begin()

    def xcopy(source, target, d):
        return pltpu.make_async_remote_copy(
            src_ref=xbuf.at[source], dst_ref=xbuf.at[source], send_sem=xsend.at[d - 1], recv_sem=xrecv.at[d - 1],
            device_id={"tp": target}, device_id_type=MESH)

    for d in range(1, groups):
        xcopy(tp, lax.rem(tp + d, groups), d).start()
    for d in range(1, groups):
        xcopy(lax.rem(tp - d + groups, groups), tp, d).wait_recv()
    squares = jnp.zeros((tokens, 1), F32)
    for t in range(groups):
        part = xbuf[t].astype(F32)
        squares = squares + jnp.sum(part * part, axis=1, keepdims=True)
        cols = slice(t * features, (t + 1) * features)
        scaled[:, cols] = (part * gain_ref[:, cols]).astype(BF16)
    row_scale = lax.rsqrt(squares / (groups * features) + EPS)

    steps(w_step, 1, outer)
    o_begin()
    w_finish()

    def project(first, size):
        total = jnp.dot(scaled[...], wbuf[:, first:first + size], preferred_element_type=F32)
        return (total * row_scale).astype(BF16)

    kvbuf[me] = project(width + 2 * conv, 2 * HEAD)
    cin[...] = project(width, conv)
    query = project(0, width)
    for head in range(heads):
        piece = query[:, head * HEAD:(head + 1) * HEAD]
        qbuf[head] = jnp.concatenate([piece, jnp.zeros_like(piece)], axis=1)

    def kvcopy(block, target, slot):
        return pltpu.make_async_remote_copy(
            src_ref=kvbuf.at[block], dst_ref=kvbuf.at[block], send_sem=ksend.at[slot], recv_sem=krecv.at[block],
            device_id={"sp": target}, device_id_type=MESH)

    def hcopy(target):
        return pltpu.make_async_remote_copy(
            src_ref=cin.at[pl.ds(tokens - 16, 16)], dst_ref=halo, send_sem=hsem.at[0], recv_sem=hsem.at[1],
            device_id={"sp": target}, device_id_type=MESH)

    def push(target, _):
        kvcopy(me, target, target).start()
        return 0

    lax.fori_loop(me + 1, n, push, 0)

    @pl.when(me < n - 1)
    def _():
        hcopy(me + 1).start()

    gate[...] = project(width + conv, conv)
    steps(o_step, 1, min(2, outer))

    row_id = lax.broadcasted_iota(jnp.int32, (tokens, tokens), 0)
    col_id = lax.broadcasted_iota(jnp.int32, (tokens, tokens), 1)
    after = jnp.where(row_id > col_id, 1.0, 0.0).astype(BF16)
    sums = jnp.concatenate([after, jnp.ones_like(after)], axis=1)

    def attend(block, diagonal):
        pair = kvbuf[block]
        for head in range(heads):
            score = lax.dot_general(qbuf[head], pair, (((1,), (1,)), ((), ())), preferred_element_type=F32)
            score = score * HEAD ** (-0.5) + bias_ref[head]
            soft = jnp.log1p(jnp.exp(-jnp.abs(score)))
            fails = -jnp.maximum(score, 0.0) - soft
            if diagonal:
                fails = jnp.where(col_id < row_id, fails, 0.0)
            high = fails.astype(BF16)
            low = (fails - high.astype(F32)).astype(BF16)
            both = jnp.dot(high, sums, preferred_element_type=F32) + jnp.dot(low, sums, preferred_element_type=F32)
            later = both[:, :tokens]
            if not diagonal:
                later = later + carry[head]
            stick = jnp.exp(jnp.minimum(score, 0.0) - soft + later)
            if diagonal:
                stick = jnp.where(col_id < row_id, stick, 0.0)
            added = jnp.dot(stick.astype(BF16), pair, preferred_element_type=F32)
            if diagonal:
                carry[head] = both[:, tokens:]
                acc[head] = added
            else:
                carry[head] += both[:, tokens:]
                acc[head] += added

    attend(me, True)

    def turn(k, _):
        block = me - k
        kvcopy(block, me, 0).wait_recv()
        attend(block, False)
        return 0

    half = (me + 2) // 2
    lax.fori_loop(1, half, turn, 0)
    steps(o_step, 2, max(2, outer // 2 + 1))
    lax.fori_loop(half, me + 1, turn, 0)
    steps(o_step, max(2, outer // 2 + 1), outer)

    for pair in range(heads // 2):
        mix[:, pair * 2 * HEAD:(pair + 1) * 2 * HEAD] = jnp.concatenate(
            [acc[2 * pair][:, HEAD:], acc[2 * pair + 1][:, HEAD:]], axis=1).astype(BF16)
    for head in range(heads):
        survival = jnp.transpose(carry[head])[0:1, :]
        lws_ref[head:head + 1, :] = jnp.log(jnp.maximum(1.0 - jnp.exp(survival), FLOOR))

    @pl.when(me == 0)
    def _():
        halo[...] = jnp.zeros_like(halo)

    @pl.when(me > 0)
    def _():
        hcopy(me).wait_recv()

    padded = jnp.concatenate([halo[...].astype(F32), cin[...].astype(F32)], axis=0)
    mixed = jnp.zeros((tokens, conv), F32)
    for tap in range(CONV_K):
        begin = 16 - (CONV_K - 1) + tap
        mixed = mixed + taps_ref[tap:tap + 1, :] * padded[begin:begin + tokens]
    mix[:, heads * HEAD:] = (gate[...].astype(F32) * mixed).astype(BF16)

    o_finish()

    def partial(target):
        def one(b, _):
            block = target * per + b
            pbuf[block] = jnp.dot(mix[...], wobuf[block], preferred_element_type=F32).astype(BF16)
            return 0

        lax.fori_loop(0, per, one, 0)

    def pcopy(target, d):
        return pltpu.make_async_remote_copy(
            src_ref=pbuf.at[pl.ds(target * per, per)], dst_ref=rbuf.at[d - 1],
            send_sem=psend.at[d - 1], recv_sem=precv.at[d - 1],
            device_id={"tp": target}, device_id_type=MESH)

    for d in (2, 1, 3) if groups == 4 else range(1, groups):
        target = lax.rem(tp + d, groups)
        partial(target)
        pcopy(target, d).start()
    partial(tp)
    for d in range(1, groups):
        pcopy(tp, d).wait_recv()

    def total(b, _):
        value = pbuf[tp * per + b].astype(F32)
        for d in range(1, groups):
            value = value + rbuf[d - 1, b].astype(F32)
        out_ref[b] = value.astype(BF16)
        return 0

    lax.fori_loop(0, per, total, 0)

    for d in range(1, groups):
        pcopy(tp, d).wait_send()
        xcopy(tp, tp, d).wait_send()

    def pushed(target, _):
        kvcopy(me, me, target).wait_send()
        return 0

    lax.fori_loop(me + 1, n, pushed, 0)

    @pl.when(me < n - 1)
    def _():
        hcopy(me).wait_send()


def local(n, groups, stream, norm_gain, w_query, w_key, w_value, w_conv_in, w_conv_gate, conv_taps, sb_bias,
          w_out_attn, w_out_conv):
    tokens, features = stream.shape
    rows, width = w_query.shape
    conv = w_conv_in.shape[1]
    heads = width // HEAD
    arows, cols = w_out_attn.shape
    inner = 2 if n % 2 == 0 else 1
    per = n // groups
    w_kv = jnp.concatenate([w_key, w_value], axis=1)
    anywhere = pl.BlockSpec(memory_space=pl.ANY)
    vmem = pl.BlockSpec(memory_space=pltpu.VMEM)
    smem = pl.BlockSpec(memory_space=pltpu.SMEM)
    dma = pltpu.SemaphoreType.DMA
    out, lws = pl.pallas_call(
        functools.partial(kernel, n, groups, inner, heads),
        out_shape=(jax.ShapeDtypeStruct((per, tokens, cols), BF16), jax.ShapeDtypeStruct((heads, tokens), F32)),
        in_specs=[smem, anywhere, vmem, vmem] + [anywhere] * 6,
        out_specs=(vmem, vmem),
        scratch_shapes=[
            pltpu.VMEM((groups, tokens, features), BF16),
            pltpu.VMEM((tokens, groups * features), BF16),
            pltpu.VMEM((n * rows, width + 2 * conv + 2 * HEAD), BF16),
            pltpu.VMEM((n, 2 * arows, cols), BF16),
            pltpu.VMEM((n, tokens, 2 * HEAD), BF16),
            pltpu.VMEM((heads, tokens, 2 * HEAD), BF16),
            pltpu.VMEM((tokens, conv), BF16),
            pltpu.VMEM((tokens, conv), BF16),
            pltpu.VMEM((16, conv), BF16),
            pltpu.VMEM((tokens, width + conv), BF16),
            pltpu.VMEM((heads, tokens, tokens), F32),
            pltpu.VMEM((heads, tokens, 2 * HEAD), F32),
            pltpu.VMEM((n, tokens, cols), BF16),
            pltpu.VMEM((groups - 1, per, tokens, cols), BF16),
            dma((7,)),
            dma((groups - 1,)), dma((groups - 1,)),
            dma((n,)), dma((n,)), dma((max(1, inner - 1), n)), dma((n,)),
            dma((n,)), dma((n,)), dma((max(1, inner - 1), n)), dma((n,)),
            dma((n,)), dma((n,)),
            dma((2,)),
            dma((groups - 1,)), dma((groups - 1,)),
        ],
        compiler_params=pltpu.CompilerParams(
            collective_id=0, has_side_effects=True, vmem_limit_bytes=60 * 1024 * 1024
        ),
        name="layer",
    )(sb_bias, stream, norm_gain[None, :], conv_taps, w_query, w_conv_in, w_conv_gate, w_kv, w_out_attn, w_out_conv)
    return out.transpose(1, 0, 2).reshape(tokens, per * cols), lws


def solution(mesh):
    placed = (
        P("sp", "tp"),
        P(),
        P("sp", "tp"),
        P("sp", "tp"),
        P("sp", "tp"),
        P("sp", "tp"),
        P("sp", "tp"),
        P(None, "tp"),
        P("tp"),
        P("tp", "sp"),
        P("tp", "sp"),
    )
    body = functools.partial(local, mesh.shape["sp"], mesh.shape["tp"])
    return jax.shard_map(
        body, mesh=mesh, in_specs=placed, out_specs=(P("sp", "tp"), P("tp", "sp")), check_vma=False
    )
```
